32 devices in a mesh: fs: 8 (over z, x), tp: 4 (over y, core).
Axes of the slice: x: 2, y: 2, z: 4, core: 2. Of those that a mesh axis runs over, the one named last changes fastest.
Arguments:
- tokens: bfloat16 [8192, 2048], P(('fs', 'tp')), may hold values from -6 to 6
- mix_gain: float32 [2048], replicated, may hold values from 0.1 to 1.9
- ffn_gain: float32 [2048], replicated, may hold values from 0.1 to 1.9
- u_weight: float32 [2048, 2048], P('fs', 'tp'), may hold values from -0.125 to 0.125
- u_scale: float32 [2048], P('tp'), may hold values from 0.5 to 2
- v_weight: float32 [2048, 2048], P('fs', 'tp'), may hold values from -0.125 to 0.125
- v_scale: float32 [2048], P('tp'), may hold values from 0.3 to 12
- v_gain: float32 [2048], P('tp'), may hold values from 0.1 to 1.9
- spatial_weight: bfloat16 [8, 128, 128], replicated, may hold values from -0.5 to 0.5
- spatial_bias: float32 [8, 128], replicated, may hold values from 0.1 to 1.9
- out_weight: float32 [2048, 2048], P('tp', 'fs'), may hold values from -0.125 to 0.125
- out_scale: float32 [2048], P('fs'), may hold values from 0.5 to 2
- gate_weight: float32 [2048, 6144], P('fs', 'tp'), may hold values from -0.125 to 0.125
- gate_scale: float32 [6144], P('tp'), may hold values from 0.5 to 2
- up_weight: float32 [2048, 6144], P('fs', 'tp'), may hold values from -0.125 to 0.125
- up_scale: float32 [6144], P('tp'), may hold values from 0.5 to 2
- down_weight: float32 [6144, 2048], P('tp', 'fs'), may hold values from -0.078125 to 0.078125
- down_scale: float32 [2048], P('fs'), may hold values from 0.5 to 2
Outputs:
- layer_out: bfloat16 [8192, 2048], P(('fs', 'tp'))
The draws below stay inside these ranges and needn't reach their ends.
All inputs are finite; a program needn't handle non-finite values.
Results may differ from the reference program's by a relative error of at most 0.02.
Values may be sent and summed in bfloat16 or wider, within the bound.
No kernel may reach another device: no remote copies, remote signals or barrier semaphores. Data moves between devices by JAX's collectives and lax.ppermute only.
A program may use at most 128 MiB of HBM per device.

```python
import math
import jax
import jax.numpy as jnp
from jax import lax

D = 2048
A = 2048
A_GROUPS = 8
BLK = 128
FF = 6144
TOKENS = 8192
N_TP = 4


def draw_v_scale(key, part):
    column_ramp = jnp.arange(A, dtype=jnp.float32) / A
    base_scale = jnp.exp(jax.random.uniform(key, (A,), jnp.float32, math.log(0.3), math.log(3.0)))
    return base_scale * 3.0 ** column_ramp


def block_levels(key, dims, split, low, largest):
    loudness, own = 1.0, jax.random.fold_in(key, 6)
    for dim, parts in split:
        heights = jnp.exp(jax.random.uniform(jax.random.fold_in(own, dim), (parts,), jnp.float32, low / len(split), largest / len(split)))
        loudness = loudness * jnp.repeat(heights, dims[dim] // parts).reshape([-1 if axis == dim else 1 for axis in range(len(dims))])
    return loudness


def centred(rng, dims, scale, reach, pieces=(), held_as=jnp.bfloat16):
    factor_of = block_levels(rng, dims, pieces, -0.22, 0.18) if pieces else 1.0
    entries = jax.random.normal(rng, dims, jnp.float32) * scale * factor_of
    return jnp.minimum(jnp.maximum(entries, -reach), reach).astype(held_as)


def setup_inputs(seed: int = 0) -> dict:
    keys = jax.random.split(jax.random.key(seed), 19)
    tokens = centred(keys[0], (TOKENS, D), 1.0, 6.0, ((0, 32),))
    mix_gain = jnp.clip(1.0 + 0.18 * jax.random.normal(keys[1], (D,), jnp.float32), 0.1, 1.9)
    ffn_gain = jnp.clip(1.0 + 0.18 * jax.random.normal(keys[2], (D,), jnp.float32), 0.1, 1.9)
    u_weight = centred(keys[3], (D, A), D ** -0.5, 0.125, ((0, 8), (1, 4)), jnp.float32)
    u_scale = jnp.clip(jnp.exp(math.log(2.0) - 1.3862944 * jax.random.uniform(keys[4], (A,), jnp.float32) ** block_levels(keys[4], (A,), ((0, 4),), -0.2, 0.2)), 0.5, 2.0)
    v_weight = centred(keys[5], (D, A), D ** -0.5, 0.125, ((0, 8), (1, 4)), jnp.float32)
    v_scale = draw_v_scale(jax.random.fold_in(keys[18], 71), 0)
    v_gain = jnp.clip(1.0 + 0.18 * jax.random.normal(keys[7], (A,), jnp.float32), 0.1, 1.9)
    spatial_weight = centred(keys[8], (A_GROUPS, BLK, BLK), BLK ** -0.5, 0.5)
    spatial_bias = jnp.clip(1.0 + 0.18 * jax.random.normal(keys[9], (A_GROUPS, BLK), jnp.float32), 0.1, 1.9)
    out_weight = centred(keys[10], (A, D), A ** -0.5, 0.125, ((0, 4), (1, 8)), jnp.float32)
    out_scale = jnp.clip(jnp.exp(math.log(2.0) - 1.3862944 * jax.random.uniform(keys[11], (D,), jnp.float32) ** block_levels(keys[11], (D,), ((0, 8),), -0.2, 0.2)), 0.5, 2.0)
    gate_weight = centred(keys[12], (D, FF), D ** -0.5, 0.125, ((0, 8), (1, 4)), jnp.float32)
    gate_scale = jnp.clip(jnp.exp(math.log(2.0) - 1.3862944 * jax.random.uniform(keys[13], (FF,), jnp.float32) ** block_levels(keys[13], (FF,), ((0, 4),), -0.2, 0.2)), 0.5, 2.0)
    up_weight = centred(keys[14], (D, FF), D ** -0.5, 0.125, ((0, 8), (1, 4)), jnp.float32)
    up_scale = jnp.clip(jnp.exp(math.log(2.0) - 1.3862944 * jax.random.uniform(keys[15], (FF,), jnp.float32) ** block_levels(keys[15], (FF,), ((0, 4),), -0.2, 0.2)), 0.5, 2.0)
    down_weight = centred(keys[16], (FF, D), FF ** -0.5, 0.078125, ((0, 4), (1, 8)), jnp.float32)
    down_scale = jnp.clip(jnp.exp(math.log(2.0) - 1.3862944 * jax.random.uniform(keys[17], (D,), jnp.float32) ** block_levels(keys[17], (D,), ((0, 8),), -0.2, 0.2)), 0.5, 2.0)
    return {"tokens": tokens, "mix_gain": mix_gain, "ffn_gain": ffn_gain, "u_weight": u_weight, "u_scale": u_scale, "v_weight": v_weight, "v_scale": v_scale, "v_gain": v_gain, "spatial_weight": spatial_weight, "spatial_bias": spatial_bias, "out_weight": out_weight, "out_scale": out_scale, "gate_weight": gate_weight, "gate_scale": gate_scale, "up_weight": up_weight, "up_scale": up_scale, "down_weight": down_weight, "down_scale": down_scale}


def rms_rows(values, norm_gain):
    widened = values.astype(jnp.float32)
    factor = lax.rsqrt(lax.optimization_barrier(jnp.mean(widened * widened, axis=1, keepdims=True)) + 1e-06)
    return (widened * factor * norm_gain).astype(jnp.bfloat16)

def project(values, matrix, scales):
    return jnp.dot(values, matrix.astype(jnp.bfloat16), preferred_element_type=jnp.float32) * scales

def run_sums(values, matrix, scales):
    run_length = values.shape[1] // N_TP
    narrow = matrix.astype(jnp.bfloat16)
    summed = jnp.zeros((values.shape[0], matrix.shape[1]), jnp.float32)
    for run_index in range(N_TP):
        lower = run_index * run_length
        partial_value = jnp.dot(values[:, lower:lower + run_length], narrow[lower:lower + run_length], preferred_element_type=jnp.float32) * scales
        summed = summed + lax.optimization_barrier(partial_value.astype(jnp.bfloat16)).astype(jnp.float32)
    return summed

def reference(tokens, mix_gain, ffn_gain, u_weight, u_scale, v_weight, v_scale, v_gain, spatial_weight, spatial_bias, out_weight, out_scale, gate_weight, gate_scale, up_weight, up_scale, down_weight, down_scale):
    normed = rms_rows(tokens, mix_gain)
    u_values = jax.nn.gelu(project(normed, u_weight, u_scale), approximate=True).astype(jnp.bfloat16)
    v_values = jax.nn.gelu(project(normed, v_weight, v_scale), approximate=True).astype(jnp.bfloat16)
    v_wide = v_values.astype(jnp.float32)
    average = lax.optimization_barrier(jnp.mean(v_wide, axis=1, keepdims=True))
    spread = lax.optimization_barrier(jnp.mean(v_wide * v_wide, axis=1, keepdims=True)) - average * average
    v_normed = ((v_wide - average) * lax.rsqrt(spread + 1e-05) * v_gain).astype(jnp.bfloat16)
    group_dim = A // A_GROUPS
    blocks = v_normed.reshape(TOKENS // BLK, BLK, A_GROUPS, group_dim).astype(jnp.float32)
    causal = jnp.tril(jnp.ones((BLK, BLK), dtype=bool))
    masked = jnp.where(causal[None], spatial_weight, jnp.zeros_like(spatial_weight)).astype(jnp.float32)
    mixed_sum = jnp.einsum('gts,bsgd->btgd', masked, blocks) + spatial_bias.T[None, :, :, None]
    gated_rows = (u_values.reshape(blocks.shape).astype(jnp.float32) * mixed_sum).astype(jnp.bfloat16)
    gated_rows = gated_rows.reshape(TOKENS, A)
    residual = (tokens.astype(jnp.float32) + run_sums(gated_rows, out_weight, out_scale)).astype(jnp.bfloat16)
    normed_second = rms_rows(residual, ffn_gain)
    hidden = (jax.nn.silu(project(normed_second, gate_weight, gate_scale)) * project(normed_second, up_weight, up_scale)).astype(jnp.bfloat16)
    return (residual.astype(jnp.float32) + run_sums(hidden, down_weight, down_scale)).astype(jnp.bfloat16)
```

```python
import jax
import jax.numpy as jnp
from jax import lax
from jax.sharding import PartitionSpec as P

A_GROUPS = 8
BLK = 128


def axis_shape(mesh):
    fs, tp = mesh.shape["fs"], mesh.shape["tp"]
    grid = mesh.devices.reshape(fs, tp)
    try:
        z = len({d.coords[2] for d in grid[:, 0]})
        y = len({d.coords[1] for d in grid[0, :]})
    except Exception:
        z, y = 4, tp // 2
    return z, fs // z, y, tp // y


def make_local(Z, X, Y, C):
    F = Z * X
    z_ring = [(z * X + x, (z + 1) % Z * X + x) for z in range(Z) for x in range(X)]
    x_ring = [(z * X + x, z * X + (x + 1) % X) for z in range(Z) for x in range(X)]

    def y_shift(k):
        return [(y * C + c, (y + k) % Y * C + c) for y in range(Y) for c in range(C)]

    def c_shift(k):
        return [(y * C + c, y * C + (c + k) % C) for y in range(Y) for c in range(C)]

    def fetch(shard, z_first=True):
        out = {}
        if z_first:
            line = [shard]
            for _ in range(Z - 1):
                line.append(lax.ppermute(line[-1], "fs", z_ring))
            for r in range(Z):
                out[r, 0] = line[r]
                for q in range(1, X):
                    out[r, q] = lax.ppermute(out[r, q - 1], "fs", x_ring)
        else:
            line = [shard]
            for _ in range(X - 1):
                line.append(lax.ppermute(line[-1], "fs", x_ring))
            for q in range(X):
                out[0, q] = line[q]
                for r in range(1, Z):
                    out[r, q] = lax.ppermute(out[r - 1, q], "fs", z_ring)
        return [out[r, q] for r in range(Z) for q in range(X)]

    def spread(rows):
        got = [rows] + [lax.ppermute(rows, "tp", y_shift(k)) for k in range(1, Y)]
        parts = []
        for g in got:
            parts.append(g)
            for k in range(1, C):
                parts.append(lax.ppermute(g, "tp", c_shift(k)))
        return jnp.concatenate(parts, axis=0)

    def scatter(part, local_rows):
        n = part.shape[1]
        view = part.reshape(Y, C, local_rows, n)
        total = view[:, 0].astype(jnp.float32)
        for k in range(1, C):
            total = total + lax.ppermute(view[:, k], "tp", c_shift(-k)).astype(jnp.float32)
        own = total[0]
        for k in range(1, Y):
            own = own + lax.ppermute(
                total[k].astype(jnp.bfloat16), "tp", y_shift(-k)
            ).astype(jnp.float32)
        return own

    def group_sum(stats):
        total = stats
        for k in range(1, C):
            total = total + jnp.roll(lax.ppermute(stats, "tp", c_shift(k)), k, axis=1)
        both = total
        for k in range(1, Y):
            total = total + jnp.roll(lax.ppermute(both, "tp", y_shift(k)), k, axis=0)
        return total

    def rms(values, gain):
        widened = values.astype(jnp.float32)
        factor = lax.rsqrt(jnp.mean(widened * widened, axis=1, keepdims=True) + 1e-06)
        return (widened * factor * gain).astype(jnp.bfloat16)

    def local(
        tokens, mix_gain, ffn_gain, u_weight, u_scale, v_weight, v_scale, v_gain,
        spatial_weight, spatial_bias, out_weight, out_scale, gate_weight, gate_scale,
        up_weight, up_scale, down_weight, down_scale,
    ):
        local_rows, D = tokens.shape
        width = D // F
        me = lax.axis_index("fs")
        mz, mx = me // X, me % X
        source = [((mz - r) % Z) * X + (mx - q) % X for r in range(Z) for q in range(X)]

        def relative(a):
            last = a.ndim - 1
            return jnp.concatenate(
                [lax.dynamic_slice_in_dim(a, s * width, width, last) for s in source], axis=last
            )

        bf = jnp.bfloat16
        u_blocks = fetch(u_weight.astype(bf))
        v_blocks = fetch(v_weight.astype(bf))
        out_blocks = fetch(out_weight.astype(bf), z_first=False)
        gate_blocks = fetch(gate_weight.astype(bf))
        up_blocks = fetch(up_weight.astype(bf))
        down_blocks = fetch(down_weight.astype(bf))
        scales = lax.all_gather(jnp.stack([out_scale, down_scale]), "fs", axis=1, tiled=True)
        gains = relative(jnp.concatenate([scales, jnp.stack([mix_gain, ffn_gain])], axis=0))
        out_columns, down_columns, mix_rel, ffn_rel = gains[0], gains[1], gains[2], gains[3]

        tokens_rel = relative(tokens)
        rows = spread(rms(tokens_rel, mix_rel))
        u_whole = jnp.concatenate(u_blocks, axis=0)
        v_whole = jnp.concatenate(v_blocks, axis=0)
        columns = u_whole.shape[1]
        v_pre = jnp.dot(rows, v_whole, preferred_element_type=jnp.float32) * v_scale
        v_values = jax.nn.gelu(v_pre, approximate=True).astype(bf)
        v_wide = v_values.astype(jnp.float32)
        sums = jnp.stack([jnp.sum(v_wide, axis=1), jnp.sum(v_wide * v_wide, axis=1)], axis=-1)
        sums = group_sum(sums.reshape(Y, C, local_rows, 2)).reshape(-1, 2)
        u_pre = jnp.dot(rows, u_whole, preferred_element_type=jnp.float32) * u_scale
        u_values = jax.nn.gelu(u_pre, approximate=True).astype(bf)
        A = columns * lax.axis_size("tp")
        average = sums[:, 0] / A
        spread_v = sums[:, 1] / A - average * average
        v_normed = (
            (v_wide - average[:, None]) * lax.rsqrt(spread_v + 1e-05)[:, None] * v_gain
        ).astype(bf)
        group_dim = A // A_GROUPS
        groups = columns // group_dim
        first_group = lax.axis_index("tp") * groups
        weights = lax.dynamic_slice_in_dim(spatial_weight, first_group, groups, 0)
        offsets = lax.dynamic_slice_in_dim(spatial_bias, first_group, groups, 0)
        causal = jnp.tril(jnp.ones((BLK, BLK), dtype=bool))
        masked = jnp.where(causal[None], weights, jnp.zeros_like(weights))
        blocks = v_normed.reshape(-1, BLK, groups, group_dim)
        mixed_sum = jnp.einsum("gts,bsgd->btgd", masked, blocks, preferred_element_type=jnp.float32)
        mixed_sum = mixed_sum + offsets.T[None, :, :, None]
        gated = (u_values.reshape(blocks.shape).astype(jnp.float32) * mixed_sum).astype(bf)
        gated = gated.reshape(-1, columns)

        out_whole = jnp.concatenate(out_blocks, axis=1)
        mix_part = jnp.dot(gated, out_whole, preferred_element_type=jnp.float32) * out_columns
        residual = (
            tokens_rel.astype(jnp.float32) + scatter(mix_part.astype(bf), local_rows)
        ).astype(bf)

        rows2 = spread(rms(residual, ffn_rel))
        gate_whole = jnp.concatenate(gate_blocks, axis=0)
        up_whole = jnp.concatenate(up_blocks, axis=0)
        gate_pre = jnp.dot(rows2, gate_whole, preferred_element_type=jnp.float32) * gate_scale
        up_pre = jnp.dot(rows2, up_whole, preferred_element_type=jnp.float32) * up_scale
        hidden = (jax.nn.silu(gate_pre) * up_pre).astype(bf)

        pieces = []
        for r in range(Z):
            piece = jnp.concatenate(down_blocks[r * X:(r + 1) * X], axis=1)
            cut = slice(r * X * width, (r + 1) * X * width)
            part = jnp.dot(hidden, piece, preferred_element_type=jnp.float32) * down_columns[cut]
            summed = scatter(part.astype(bf), local_rows)
            pieces.append((residual[:, cut].astype(jnp.float32) + summed).astype(bf))
        final = jnp.concatenate(pieces, axis=1)
        back = [((mz - z) % Z) * X + (mx - x) % X for z in range(Z) for x in range(X)]
        return jnp.concatenate(
            [lax.dynamic_slice_in_dim(final, b * width, width, 1) for b in back], axis=1
        )

    return local


def solution(mesh):
    placed = (
        P(("fs", "tp"), None), P(), P(), P("fs", "tp"), P("tp"), P("fs", "tp"), P("tp"), P("tp"),
        P(), P(), P("tp", "fs"), P("fs"), P("fs", "tp"), P("tp"), P("fs", "tp"), P("tp"),
        P("tp", "fs"), P("fs"),
    )
    return jax.shard_map(
        make_local(*axis_shape(mesh)),
        mesh=mesh, in_specs=placed, out_specs=P(("fs", "tp"), None), check_vma=False,
    )
```
